32 devices in a mesh: sp: 8 (over z, y), tp: 4 (over x, core).
Axes of the slice: x: 2, y: 2, z: 4, core: 2. Of those that a mesh axis runs over, the one named last changes fastest.
Arguments:
- tokens: bfloat16 [3072, 2048], P(('sp', 'tp')), may hold values from -60 to 60
- query_weight: bfloat16 [2048, 1024], P(None, 'tp'), may hold values from -0.125 to 0.125
- key_weight: bfloat16 [2048, 1024], P(None, 'tp'), may hold values from -0.125 to 0.125
- value_weight: bfloat16 [2048, 1024], P(None, 'tp'), may hold values from -0.125 to 0.125
- outer_gate: bfloat16 [2048, 1024], P(None, 'tp'), may hold values from -0.125 to 0.125
- inner_gate: bfloat16 [2048, 1024], P(None, 'tp'), may hold values from -0.125 to 0.125
- conv_weight: bfloat16 [2048, 1024], P(None, 'tp'), may hold values from -0.125 to 0.125
- conv_taps: bfloat16 [3, 1024], P(None, 'tp'), may hold values from -3 to 3
- gate_sum: float32 [8, 3072], P('tp'), may hold values from -180 to 0, as said below
- head_gain: bfloat16 [1024], P('tp'), may hold values from 0.099609375 to 1.8984375
- channel_gain: bfloat16 [1024], P('tp'), may hold values from 0.099609375 to 1.8984375
- attention_out: bfloat16 [1024, 2048], P('tp'), may hold values from -0.125 to 0.125
- channel_out: bfloat16 [1024, 2048], P('tp'), may hold values from -0.125 to 0.125
Outputs:
- mixed_out: bfloat16 [3072, 2048], P(('sp', 'tp'))
The draws below stay inside these ranges and needn't reach their ends.
Inputs may be any that keep to these rules, and one draw needn't show every extreme that they name: gate_sum[h, t] never rises with t.
All inputs are finite; a program needn't handle non-finite values.
Results may differ from the reference program's by a relative error of at most 0.015.
Values may be sent and summed in bfloat16 or wider, within the bound.
A program may use at most 192 MiB of HBM per device.

```python
import math
import jax
import jax.numpy as jnp
from jax import lax

D = 2048
ATTENTION_HEADS = 8
HEAD = 128
KTAP = 3
TOK_DEV = 384
AW = 1024
CW = 1024
SEQUENCE_TOKENS = 3072


def draw_tokens(key, part):
    key_sequence = jax.random.split(jax.random.fold_in(key, 7), 6)
    return jnp.clip(jax.random.normal(key_sequence[5], (SEQUENCE_TOKENS, D), jnp.float32), -6.0, 6.0).astype(jnp.bfloat16)


def draw_gate_sum(key, part):
    key_sequence = jax.random.split(jax.random.fold_in(key, 11), 5)
    head_order = jax.random.permutation(key_sequence[0], ATTENTION_HEADS)
    quick_decay_heads = head_order < ATTENTION_HEADS // 2
    jitter = jax.random.uniform(key_sequence[1], (ATTENTION_HEADS, SEQUENCE_TOKENS), jnp.float32, 0.25, 1.75)
    block_rates = jnp.exp(jax.random.uniform(key_sequence[2], (SEQUENCE_TOKENS // TOK_DEV,), jnp.float32, math.log(0.5), math.log(2.0)))
    position_rates = jnp.repeat(block_rates, TOK_DEV)
    forget_rates = jnp.where(quick_decay_heads[:, None], 6.0 / TOK_DEV, 0.5 / SEQUENCE_TOKENS) * jitter * position_rates[None, :]
    cluster_position = jax.random.randint(key_sequence[3], (ATTENTION_HEADS, 3), 0, SEQUENCE_TOKENS)
    cluster_length = jax.random.uniform(key_sequence[4], (ATTENTION_HEADS, 3), jnp.float32, math.log(0.5), math.log(0.8))
    token_positions = jnp.arange(SEQUENCE_TOKENS)
    cluster_match = token_positions[None, None, :] == cluster_position[:, :, None]
    token_clusters = jnp.sum(jnp.where(cluster_match, cluster_length[:, :, None], 0.0), axis=1)
    token_clusters = jnp.where(quick_decay_heads[:, None], 0.0, token_clusters)
    return jnp.cumsum(token_clusters - forget_rates, axis=1)


def shard_levels(rng, extent, cuts, least, largest):
    factor_of, own = 1.0, jax.random.fold_in(rng, 6)
    for dim, shards_of in cuts:
        heights = jnp.exp(jax.random.uniform(jax.random.fold_in(own, dim), (shards_of,), jnp.float32, least / len(cuts), largest / len(cuts)))
        factor_of = factor_of * jnp.repeat(heights, extent[dim] // shards_of).reshape([-1 if axis == dim else 1 for axis in range(len(extent))])
    return factor_of


def scatter_about(rng, extent, deviation, most, cuts=(), held_as=jnp.bfloat16):
    level = shard_levels(rng, extent, cuts, -0.22, 0.18) if cuts else 1.0
    array = jax.random.normal(rng, extent, jnp.float32) * deviation * level
    return jnp.minimum(jnp.maximum(array, -most), most).astype(held_as)


def setup_inputs(seed: int = 0) -> dict:
    keys = jax.random.split(jax.random.key(seed), 14)
    tokens = draw_tokens(jax.random.fold_in(keys[13], 71), 0)
    query_weight = scatter_about(keys[1], (D, AW), D ** -0.5, 0.125, ((1, 4),))
    key_weight = scatter_about(keys[2], (D, AW), D ** -0.5, 0.125, ((1, 4),))
    value_weight = scatter_about(keys[3], (D, AW), D ** -0.5, 0.125, ((1, 4),))
    outer_gate = scatter_about(keys[4], (D, CW), D ** -0.5, 0.125, ((1, 4),))
    inner_gate = scatter_about(keys[5], (D, CW), D ** -0.5, 0.125, ((1, 4),))
    conv_weight = scatter_about(keys[6], (D, CW), D ** -0.5, 0.125, ((1, 4),))
    conv_taps = scatter_about(keys[7], (KTAP, CW), 0.577, 3.0, ((1, 4),))
    gate_sum = draw_gate_sum(jax.random.fold_in(keys[13], 71), 0)
    head_gain = jnp.clip(1.0 + 0.18 * jax.random.normal(keys[9], (AW,), jnp.float32), 0.099609375, 1.8984375).astype(jnp.bfloat16)
    channel_gain = jnp.clip(1.0 + 0.18 * jax.random.normal(keys[10], (CW,), jnp.float32), 0.099609375, 1.8984375).astype(jnp.bfloat16)
    attention_out = scatter_about(keys[11], (AW, D), (AW + CW) ** -0.5, 0.125, ((0, 4),))
    channel_out = scatter_about(keys[12], (CW, D), (AW + CW) ** -0.5, 0.125, ((0, 4),))
    return {"tokens": tokens, "query_weight": query_weight, "key_weight": key_weight, "value_weight": value_weight, "outer_gate": outer_gate, "inner_gate": inner_gate, "conv_weight": conv_weight, "conv_taps": conv_taps, "gate_sum": gate_sum, "head_gain": head_gain, "channel_gain": channel_gain, "attention_out": attention_out, "channel_out": channel_out}


def project_rows(tokens, weight):
    return jnp.dot(tokens, weight, preferred_element_type=jnp.float32).astype(jnp.bfloat16)

def head_norm(values, gain_vector):
    row_count = values.shape[0]
    shaped = values.reshape(row_count, -1, HEAD)
    shaped = shaped * lax.rsqrt(lax.optimization_barrier(jnp.mean(shaped * shaped, axis=-1, keepdims=True)) + 1e-06)
    return (shaped.reshape(row_count, -1) * gain_vector.astype(jnp.float32)).astype(jnp.bfloat16)

def reference(tokens, query_weight, key_weight, value_weight, outer_gate, inner_gate, conv_weight, conv_taps, gate_sum, head_gain, channel_gain, attention_out, channel_out):
    queries = project_rows(tokens, query_weight)
    keys_all = project_rows(tokens, key_weight)
    values_all = project_rows(tokens, value_weight)
    gate_outer = project_rows(tokens, outer_gate)
    gate_inner = project_rows(tokens, inner_gate)
    conv_input = project_rows(tokens, conv_weight)
    mixed_in = (gate_inner.astype(jnp.float32) * conv_input.astype(jnp.float32)).astype(jnp.bfloat16)
    padded = jnp.concatenate([jnp.zeros((KTAP - 1, CW), jnp.float32), mixed_in.astype(jnp.float32)], axis=0)
    summed = jnp.zeros((SEQUENCE_TOKENS, CW), jnp.float32)
    for offset in range(KTAP):
        summed = summed + conv_taps[offset].astype(jnp.float32) * padded[offset:offset + SEQUENCE_TOKENS]
    conv_out = gate_outer.astype(jnp.float32) * summed
    block_rows = math.gcd(SEQUENCE_TOKENS, 512)
    query_heads = queries.reshape(SEQUENCE_TOKENS, ATTENTION_HEADS, HEAD).astype(jnp.float32)
    key_heads = keys_all.reshape(SEQUENCE_TOKENS, ATTENTION_HEADS, HEAD).astype(jnp.float32)
    value_heads = values_all.reshape(SEQUENCE_TOKENS, ATTENTION_HEADS, HEAD).astype(jnp.float32)
    score_scale = HEAD ** (-0.5)
    token_positions = jnp.arange(SEQUENCE_TOKENS, dtype=jnp.int32)

    def attend(block_index):
        first_row = (block_index * block_rows).astype(jnp.int32)
        query_block = lax.dynamic_slice_in_dim(query_heads, first_row, block_rows, 0)
        gate_block = lax.dynamic_slice_in_dim(gate_sum, first_row, block_rows, 1)
        query_pos = first_row + jnp.arange(block_rows, dtype=jnp.int32)
        logits = jnp.einsum('qhd,khd->qhk', query_block, key_heads) * score_scale
        logits = logits + gate_block.T[:, :, None] - gate_sum[None, :, :]
        allowed = (token_positions[None, :] <= query_pos[:, None])[:, None, :]
        logits = jnp.where(allowed, logits, -jnp.inf)
        peak = lax.optimization_barrier(jnp.max(logits, axis=-1, keepdims=True))
        weights = jnp.exp(logits - peak)
        total = lax.optimization_barrier(jnp.sum(weights, axis=-1))
        rounded = lax.optimization_barrier(weights.astype(jnp.bfloat16))
        mixed = jnp.einsum('qhk,khd->qhd', rounded.astype(jnp.float32), value_heads)
        return mixed / total[..., None]
    blocks = lax.map(attend, jnp.arange(SEQUENCE_TOKENS // block_rows, dtype=jnp.int32))
    attention = blocks.reshape(SEQUENCE_TOKENS, ATTENTION_HEADS * HEAD)
    head_normed = head_norm(attention, head_gain)
    group_normed = head_norm(conv_out, channel_gain)
    total_out = jnp.dot(head_normed, attention_out, preferred_element_type=jnp.float32) + jnp.dot(group_normed, channel_out, preferred_element_type=jnp.float32)
    return total_out.astype(jnp.bfloat16)
```

```python
import functools
import math

import jax
import jax.numpy as jnp
from jax import lax
from jax.experimental import pallas as pl
from jax.experimental.pallas import tpu as pltpu
from jax.sharding import PartitionSpec as P

HEAD = 128
KTAP = 3
HALO = 16
MESH = pl.DeviceIdType.MESH
F32 = jnp.float32
BF16 = jnp.bfloat16


def rms(values, gain):
    scale = lax.rsqrt(jnp.mean(values * values, axis=-1, keepdims=True) + 1e-06)
    return (values * scale * gain).astype(BF16)


def kernel(
    S,
    T,
    tokens,
    wq,
    wk,
    wv,
    wgo,
    wgi,
    wci,
    taps,
    gate,
    head_gain,
    channel_gain,
    wattn,
    wchan,
    out,
    tok,
    w,
    wo,
    kv,
    qbuf,
    stage_kv,
    stage_q,
    gates,
    mixed,
    halo,
    padded,
    group,
    peak,
    total,
    acc,
    ret,
    heads,
    part,
    part_in,
    xsum,
    xsum_in,
    w_sem,
    wo_sem,
    tok_sem,
    tok_send,
    tok_recv,
    y_send,
    y_recv,
    kv_send,
    kv_far,
    kv_recv,
    halo_send,
    halo_recv,
    ret_send,
    ret_recv,
    pair_send,
    pair_recv,
    x_send,
    x_recv,
):
    sp = lax.axis_index("sp")
    tp = lax.axis_index("tp")
    G = S // 2
    g = sp // 2
    par = sp % 2
    mate = sp + 1 - 2 * par
    C = tokens.shape[0]
    R = C * T
    HR = R // 2
    R2 = 2 * R
    pair = tp // 2
    tp1 = tp + 1 - 2 * (tp % 2)
    tp2 = (tp + 2) % T
    tp3 = (tp1 + 2) % T
    near = G // 2

    weights = (wk, wv, wq, wgi, wci, wgo)
    own_copy = pltpu.make_async_copy(tokens, tok.at[pl.ds(tp * C, C)], tok_sem)
    own_copy.start()
    w_copies = [pltpu.make_async_copy(weights[i], w.at[i], w_sem.at[i]) for i in range(6)]
    for copy in w_copies:
        copy.start()
    wo_copies = [
        pltpu.make_async_copy(ref, wo.at[i], wo_sem.at[i]) for i, ref in enumerate((wattn, wchan))
    ]
    for copy in wo_copies:
        copy.start()

    barrier = pltpu.get_barrier_semaphore()
    for o in range(1, T):
        pl.semaphore_signal(barrier, inc=1, device_id={"tp": (tp + o) % T}, device_id_type=MESH)
    for o in range(1, S):
        pl.semaphore_signal(barrier, inc=1, device_id={"sp": (sp + o) % S}, device_id_type=MESH)
    pl.semaphore_wait(barrier, S + T - 2)

    def tok_copy(slot, target, index):
        rows = pl.ds(slot * C, C)
        return pltpu.make_async_remote_copy(
            src_ref=tok.at[rows],
            dst_ref=tok.at[rows],
            send_sem=tok_send.at[index],
            recv_sem=tok_recv.at[index],
            device_id={"tp": target},
            device_id_type=MESH,
        )

    own_copy.wait()
    cross = tok_copy(tp, tp2, 0)
    cross.start()
    beside = tok_copy(tp, tp1, 1)
    beside.start()

    def half_start(half):
        return (pair if half == 0 else 1 - pair) * HR

    def y_kv(half):
        rs = half_start(half)
        return pltpu.make_async_remote_copy(
            src_ref=stage_kv.at[:, pl.ds(rs, HR), :],
            dst_ref=kv.at[g, :, pl.ds(par * R + rs, HR), :],
            send_sem=y_send.at[half, 0],
            recv_sem=y_recv.at[half, 0],
            device_id={"sp": mate},
            device_id_type=MESH,
        )

    def y_q(half):
        rs = half_start(half)
        return pltpu.make_async_remote_copy(
            src_ref=stage_q.at[pl.ds(rs, HR), :],
            dst_ref=qbuf.at[pl.ds(par * R + rs, HR), :],
            send_sem=y_send.at[half, 1],
            recv_sem=y_recv.at[half, 1],
            device_id={"sp": mate},
            device_id_type=MESH,
        )

    def piece_copy(d, p, step, send_sem):
        half, other = p // 2, p % 2
        rows = pl.ds((1 - par if other else par) * R + half_start(half), HR)
        ref = kv.at[g - d, :, rows, :]
        return pltpu.make_async_remote_copy(
            src_ref=ref,
            dst_ref=ref,
            send_sem=send_sem,
            recv_sem=kv_recv.at[d + step, p],
            device_id={"sp": lax.rem(sp + 2 * step, S)},
            device_id_type=MESH,
        )

    def send_own(p):
        @pl.when(g + 1 < G)
        def _():
            piece_copy(0, p, 1, kv_send.at[0, p]).start()

        for step in range(near + 1, G):

            @pl.when(g + step < G)
            def _():
                piece_copy(0, p, step, kv_far.at[step, p]).start()

    def project(half, index):
        rs = pl.multiple_of(half_start(half), 16)
        rows = tok[pl.ds(rs, HR), :]
        return rs, jnp.dot(rows, w[index], preferred_element_type=F32).astype(BF16)

    def split(value):
        a, b = value[:, :HEAD], value[:, HEAD:]
        return jnp.where(par == 0, a, b), jnp.where(par == 0, b, a)

    def attention_inputs(half):
        for i in range(2):
            if half == 0:
                w_copies[i].wait()
            rs, value = project(half, i)
            mine, theirs = split(value)
            kv[g, i, pl.ds(pl.multiple_of(par * R + rs, 16), HR), :] = mine
            stage_kv[i, pl.ds(rs, HR), :] = theirs
        y_kv(half).start()
        send_own(2 * half)
        if half == 0:
            w_copies[2].wait()
        rs, value = project(half, 2)
        mine, theirs = split(value)
        qbuf[pl.ds(pl.multiple_of(par * R + rs, 16), HR), :] = mine
        stage_q[pl.ds(rs, HR), :] = theirs
        y_q(half).start()

    def gate_inputs(half):
        for i in range(3, 6):
            if half == 0:
                w_copies[i].wait()
            rs, value = project(half, i)
            gates[i - 3, pl.ds(rs, HR), :] = value

    beside.wait_recv()
    attention_inputs(0)
    gate_inputs(0)
    y_kv(0).wait_recv()
    send_own(1)

    tok_copy(tp2, tp2, 0).wait_recv()
    onward = tok_copy(tp2, tp1, 2)
    onward.start()
    tok_copy(tp3, tp1, 2).wait_recv()
    attention_inputs(1)
    gate_inputs(1)
    y_kv(1).wait_recv()
    send_own(3)

    mixed[...] = (gates[0].astype(F32) * gates[1].astype(F32)).astype(BF16)
    halo_copy = pltpu.make_async_remote_copy(
        src_ref=mixed.at[pl.ds(R - HALO, HALO), :],
        dst_ref=halo,
        send_sem=halo_send,
        recv_sem=halo_recv,
        device_id={"sp": lax.rem(sp + 1, S)},
        device_id_type=MESH,
    )

    @pl.when(sp + 1 < S)
    def _():
        halo_copy.start()

    y_q(0).wait_recv()
    y_q(1).wait_recv()

    log2e = math.log2(math.e)
    coefficient = log2e * HEAD ** (-0.5)
    QT = 256 if R2 % 256 == 0 else 128

    def attend(b, diagonal):
        bias = gate[pl.ds(par, 1), pl.ds(pl.multiple_of(b * R2, 128), R2)] * log2e
        for start in range(0, R2, QT):
            stop = start + QT if diagonal else R2
            rows = pl.ds(start, QT)
            s = lax.dot_general(
                qbuf[rows, :],
                kv[b, 0, pl.ds(0, stop), :],
                (((1,), (1,)), ((), ())),
                preferred_element_type=F32,
            )
            s = s * coefficient - bias[:, :stop]
            if diagonal:
                row = lax.broadcasted_iota(jnp.int32, s.shape, 0) + start
                col = lax.broadcasted_iota(jnp.int32, s.shape, 1)
                s = jnp.where(col <= row, s, -jnp.inf)
                top = jnp.max(s, axis=-1, keepdims=True)
            else:
                before = peak[rows, :]
                top = jnp.maximum(before, jnp.max(s, axis=-1, keepdims=True))
            weight = jnp.exp2(s - top)
            norm = jnp.sum(weight, axis=-1, keepdims=True)
            value = jnp.dot(
                weight.astype(BF16), kv[b, 1, pl.ds(0, stop), :], preferred_element_type=F32
            )
            if not diagonal:
                fade = jnp.exp2(before - top)
                norm = norm + total[rows, :] * fade
                value = value + acc[rows, :] * fade
            peak[rows, :] = top
            total[rows, :] = norm
            acc[rows, :] = value

    attend(g, True)

    @pl.when(sp > 0)
    def _():
        halo_copy.wait_recv()
        padded[0:8, :] = halo[HALO - 8 : HALO, :].astype(F32)

    @pl.when(sp == 0)
    def _():
        padded[0:8, :] = jnp.zeros((8, padded.shape[1]), F32)

    padded[pl.ds(8, R), :] = mixed[...].astype(F32)
    summed = jnp.zeros(mixed.shape, F32)
    for j in range(KTAP):
        summed = summed + taps[j : j + 1, :].astype(F32) * padded[pl.ds(9 - KTAP + j, R), :]
    conv_out = gates[2].astype(F32) * summed
    for h in range(conv_out.shape[1] // HEAD):
        cols = slice(h * HEAD, (h + 1) * HEAD)
        group[:, cols] = rms(conv_out[:, cols], channel_gain[:, cols].astype(F32))

    def chain(d, carry):
        for p in range(4):
            piece_copy(d - 1, p, 1, kv_send.at[0, p]).wait_recv()

            @pl.when((d < near) & (g + 1 < G))
            def _():
                piece_copy(d, p, 1, kv_send.at[d, p]).start()

        attend(g - d, False)
        return carry

    lax.fori_loop(1, g + 1, chain, 0)

    gain = jnp.where(par == 0, head_gain[:, :HEAD], head_gain[:, HEAD:]).astype(F32)

    def finished(first):
        rows = pl.ds(pl.multiple_of(first, 16), R)
        return rms(acc[rows, :] / total[rows, :], gain)

    ret[...] = finished((1 - par) * R)
    back = pltpu.make_async_remote_copy(
        src_ref=ret,
        dst_ref=heads.at[par],
        send_sem=ret_send,
        recv_sem=ret_recv,
        device_id={"sp": mate},
        device_id_type=MESH,
    )
    back.start()
    heads[par] = finished(par * R)
    for copy in wo_copies:
        copy.wait()
    back.wait_recv()

    NH = out.shape[1] // 2

    def partial(chunk, n):
        rows = pl.ds(pl.multiple_of(chunk * C, 16), C)
        both = jnp.concatenate([heads[0, rows, :], heads[1, rows, :]], axis=1)
        cols = pl.ds(n * NH, NH)
        return jnp.dot(both, wo[0, :, cols], preferred_element_type=F32) + jnp.dot(
            group[rows, :], wo[1, :, cols], preferred_element_type=F32
        )

    def pair_copy(i, n):
        return pltpu.make_async_remote_copy(
            src_ref=part.at[i, n],
            dst_ref=part_in.at[i, n],
            send_sem=pair_send.at[i, n],
            recv_sem=pair_recv.at[i, n],
            device_id={"tp": tp1},
            device_id_type=MESH,
        )

    def x_copy(n):
        return pltpu.make_async_remote_copy(
            src_ref=xsum.at[n],
            dst_ref=xsum_in.at[n],
            send_sem=x_send.at[n],
            recv_sem=x_recv.at[n],
            device_id={"tp": tp2},
            device_id_type=MESH,
        )

    for n in range(2):
        part[0, n] = partial(tp3, n).astype(BF16)
        pair_copy(0, n).start()
    for n in range(2):
        value = partial(tp2, n)
        pair_copy(0, n).wait_recv()
        xsum[n] = (value + part_in[0, n].astype(F32)).astype(BF16)
        x_copy(n).start()
    for n in range(2):
        part[1, n] = partial(tp1, n).astype(BF16)
        pair_copy(1, n).start()
    for n in range(2):
        value = partial(tp, n)
        pair_copy(1, n).wait_recv()
        value = value + part_in[1, n].astype(F32)
        x_copy(n).wait_recv()
        out[:, pl.ds(n * NH, NH)] = (value + xsum_in[n].astype(F32)).astype(BF16)

    cross.wait_send()
    beside.wait_send()
    onward.wait_send()
    for half in range(2):
        y_kv(half).wait_send()
        y_q(half).wait_send()
    back.wait_send()

    @pl.when(sp + 1 < S)
    def _():
        halo_copy.wait_send()

    for n in range(2):
        x_copy(n).wait_send()
        for i in range(2):
            pair_copy(i, n).wait_send()
    for p in range(4):

        @pl.when(g + 1 < G)
        def _():
            piece_copy(0, p, 1, kv_send.at[0, p]).wait_send()

        for d in range(1, near):

            @pl.when((g + 1 < G) & (g >= d))
            def _():
                piece_copy(d, p, 1, kv_send.at[d, p]).wait_send()

        for step in range(near + 1, G):

            @pl.when(g + step < G)
            def _():
                piece_copy(0, p, step, kv_far.at[step, p]).wait_send()


def local(S, T, tokens, *rest):
    (wq, wk, wv, wgo, wgi, wci, taps, gate, head_gain, channel_gain, wattn, wchan) = rest
    C, D = tokens.shape
    R = C * T
    A = wq.shape[1]
    G = S // 2
    N = wattn.shape[1]
    hbm = pl.BlockSpec(memory_space=pl.ANY)
    vmem = pl.BlockSpec(memory_space=pltpu.VMEM)
    dma = pltpu.SemaphoreType.DMA
    return pl.pallas_call(
        functools.partial(kernel, S, T),
        out_shape=jax.ShapeDtypeStruct((C, N), BF16),
        in_specs=[hbm] * 7 + [vmem] * 4 + [hbm] * 2,
        out_specs=vmem,
        scratch_shapes=[
            pltpu.VMEM((R, D), BF16),
            pltpu.VMEM((6, D, A), BF16),
            pltpu.VMEM((2, A, N), BF16),
            pltpu.VMEM((G, 2, 2 * R, HEAD), BF16),
            pltpu.VMEM((2 * R, HEAD), BF16),
            pltpu.VMEM((2, R, HEAD), BF16),
            pltpu.VMEM((R, HEAD), BF16),
            pltpu.VMEM((3, R, A), BF16),
            pltpu.VMEM((R, A), BF16),
            pltpu.VMEM((HALO, A), BF16),
            pltpu.VMEM((R + 8, A), F32),
            pltpu.VMEM((R, A), BF16),
            pltpu.VMEM((2 * R, 1), F32),
            pltpu.VMEM((2 * R, 1), F32),
            pltpu.VMEM((2 * R, HEAD), F32),
            pltpu.VMEM((R, HEAD), BF16),
            pltpu.VMEM((2, R, HEAD), BF16),
            pltpu.VMEM((2, 2, C, N // 2), BF16),
            pltpu.VMEM((2, 2, C, N // 2), BF16),
            pltpu.VMEM((2, C, N // 2), BF16),
            pltpu.VMEM((2, C, N // 2), BF16),
            dma((6,)),
            dma((2,)),
            dma,
            dma((3,)),
            dma((3,)),
            dma((2, 2)),
            dma((2, 2)),
            dma((G, 4)),
            dma((G, 4)),
            dma((G + 1, 4)),
            dma,
            dma,
            dma,
            dma,
            dma((2, 2)),
            dma((2, 2)),
            dma((2,)),
            dma((2,)),
        ],
        compiler_params=pltpu.CompilerParams(
            collective_id=0, has_side_effects=True, vmem_limit_bytes=60 * 1024 * 1024
        ),
    )(
        tokens,
        wq,
        wk,
        wv,
        wgo,
        wgi,
        wci,
        taps,
        gate,
        head_gain.reshape(1, A),
        channel_gain.reshape(1, A),
        wattn,
        wchan,
    )


def solution(mesh):
    S, T = mesh.shape["sp"], mesh.shape["tp"]
    cols = P(None, "tp")
    rows = P("tp", None)
    placed = (
        (P(("sp", "tp"), None),) + (cols,) * 7 + (rows, P("tp"), P("tp")) + (rows, rows)
    )
    return jax.shard_map(
        functools.partial(local, S, T),
        mesh=mesh,
        in_specs=placed,
        out_specs=P(("sp", "tp"), None),
        check_vma=False,
    )
```

```python
import functools
import math

import jax
import jax.numpy as jnp
from jax import lax
from jax.experimental import pallas as pl
from jax.experimental.pallas import tpu as pltpu
from jax.sharding import PartitionSpec as P

HEAD = 128
KTAP = 3
HALO = 16
MESH = pl.DeviceIdType.MESH
F32 = jnp.float32
BF16 = jnp.bfloat16


def rms(values, gain):
    scale = lax.rsqrt(jnp.mean(values * values, axis=-1, keepdims=True) + 1e-06)
    return (values * scale * gain).astype(BF16)


def kernel(
    S,
    T,
    tokens,
    wq,
    wk,
    wv,
    wgo,
    wgi,
    wci,
    taps,
    gate,
    head_gain,
    channel_gain,
    wattn,
    wchan,
    out,
    tok,
    w,
    wo,
    kv,
    qbuf,
    stage_kv,
    stage_q,
    gates,
    mixed,
    halo,
    padded,
    group,
    peak,
    total,
    acc,
    ret,
    heads,
    part,
    part_in,
    xsum,
    xsum_in,
    w_sem,
    wo_sem,
    tok_sem,
    tok_send,
    tok_recv,
    y_send,
    y_recv,
    kv_send,
    kv_far,
    kv_recv,
    halo_send,
    halo_recv,
    ret_send,
    ret_recv,
    pair_send,
    pair_recv,
    x_send,
    x_recv,
):
    sp = lax.axis_index("sp")
    tp = lax.axis_index("tp")
    G = S // 2
    g = sp // 2
    par = sp % 2
    mate = sp + 1 - 2 * par
    C = tokens.shape[0]
    R = C * T
    HR = R // 2
    R2 = 2 * R
    pair = tp // 2
    tp1 = tp + 1 - 2 * (tp % 2)
    tp2 = (tp + 2) % T
    tp3 = (tp1 + 2) % T
    near = G // 2

    weights = (wk, wv, wq, wgi, wci, wgo)
    own_copy = pltpu.make_async_copy(tokens, tok.at[pl.ds(tp * C, C)], tok_sem)
    own_copy.start()
    w_copies = [pltpu.make_async_copy(weights[i], w.at[i], w_sem.at[i]) for i in range(6)]
    for copy in w_copies[:3]:
        copy.start()
    wo_copies = [
        pltpu.make_async_copy(ref, wo.at[i], wo_sem.at[i]) for i, ref in enumerate((wattn, wchan))
    ]

    barrier = pltpu.get_barrier_semaphore()
    for o in range(1, T):
        pl.semaphore_signal(barrier, inc=1, device_id={"tp": (tp + o) % T}, device_id_type=MESH)
    for o in range(1, S):
        pl.semaphore_signal(barrier, inc=1, device_id={"sp": (sp + o) % S}, device_id_type=MESH)
    pl.semaphore_wait(barrier, S + T - 2)

    def tok_copy(slot, target, index):
        rows = pl.ds(slot * C, C)
        return pltpu.make_async_remote_copy(
            src_ref=tok.at[rows],
            dst_ref=tok.at[rows],
            send_sem=tok_send.at[index],
            recv_sem=tok_recv.at[index],
            device_id={"tp": target},
            device_id_type=MESH,
        )

    own_copy.wait()
    cross = tok_copy(tp, tp2, 0)
    cross.start()
    beside = tok_copy(tp, tp1, 1)
    beside.start()
    for copy in w_copies[3:] + wo_copies:
        copy.start()

    def half_start(half):
        return (pair if half == 0 else 1 - pair) * HR

    def y_kv(half):
        rs = half_start(half)
        return pltpu.make_async_remote_copy(
            src_ref=stage_kv.at[:, pl.ds(rs, HR), :],
            dst_ref=kv.at[g, :, pl.ds(par * R + rs, HR), :],
            send_sem=y_send.at[half, 0],
            recv_sem=y_recv.at[half, 0],
            device_id={"sp": mate},
            device_id_type=MESH,
        )

    def y_q(half):
        rs = half_start(half)
        return pltpu.make_async_remote_copy(
            src_ref=stage_q.at[pl.ds(rs, HR), :],
            dst_ref=qbuf.at[pl.ds(par * R + rs, HR), :],
            send_sem=y_send.at[half, 1],
            recv_sem=y_recv.at[half, 1],
            device_id={"sp": mate},
            device_id_type=MESH,
        )

    def piece_copy(d, p, step, send_sem):
        half, other = p // 2, p % 2
        rows = pl.ds((1 - par if other else par) * R + half_start(half), HR)
        ref = kv.at[g - d, :, rows, :]
        return pltpu.make_async_remote_copy(
            src_ref=ref,
            dst_ref=ref,
            send_sem=send_sem,
            recv_sem=kv_recv.at[d + step, p],
            device_id={"sp": lax.rem(sp + 2 * step, S)},
            device_id_type=MESH,
        )

    def send_own(p):
        @pl.when(g + 1 < G)
        def _():
            piece_copy(0, p, 1, kv_send.at[0, p]).start()

        for step in range(near + 1, G):

            @pl.when(g + step < G)
            def _():
                piece_copy(0, p, step, kv_far.at[step, p]).start()

    def arrived(d, p, send_on):
        piece_copy(d, p, 0, kv_send.at[d, p]).wait_recv()

        @pl.when(jnp.logical_and(send_on, g + 1 < G))
        def _():
            piece_copy(d, p, 1, kv_send.at[d, p]).start()

    def arrived_near(p):
        @pl.when(g > 0)
        def _():
            arrived(1, p, near > 1)

    def project(half, index):
        rs = pl.multiple_of(half_start(half), 16)
        rows = tok[pl.ds(rs, HR), :]
        return rs, jnp.dot(rows, w[index], preferred_element_type=F32).astype(BF16)

    def split(value):
        a, b = value[:, :HEAD], value[:, HEAD:]
        return jnp.where(par == 0, a, b), jnp.where(par == 0, b, a)

    def attention_inputs(half):
        for i in range(2):
            if half == 0:
                w_copies[i].wait()
            rs, value = project(half, i)
            mine, theirs = split(value)
            kv[g, i, pl.ds(pl.multiple_of(par * R + rs, 16), HR), :] = mine
            stage_kv[i, pl.ds(rs, HR), :] = theirs
        y_kv(half).start()
        send_own(2 * half)
        if half == 0:
            w_copies[2].wait()
        rs, value = project(half, 2)
        mine, theirs = split(value)
        qbuf[pl.ds(pl.multiple_of(par * R + rs, 16), HR), :] = mine
        stage_q[pl.ds(rs, HR), :] = theirs
        y_q(half).start()

    def gate_inputs(half):
        for i in range(3, 6):
            if half == 0:
                w_copies[i].wait()
            rs, value = project(half, i)
            gates[i - 3, pl.ds(rs, HR), :] = value

    beside.wait_recv()
    attention_inputs(0)
    gate_inputs(0)
    y_kv(0).wait_recv()
    send_own(1)
    arrived_near(0)

    tok_copy(tp2, tp2, 0).wait_recv()
    onward = tok_copy(tp2, tp1, 2)
    onward.start()
    tok_copy(tp3, tp1, 2).wait_recv()
    attention_inputs(1)
    arrived_near(1)
    gate_inputs(1)
    y_kv(1).wait_recv()
    send_own(3)
    arrived_near(2)

    mixed[...] = (gates[0].astype(F32) * gates[1].astype(F32)).astype(BF16)
    halo_copy = pltpu.make_async_remote_copy(
        src_ref=mixed.at[pl.ds(R - HALO, HALO), :],
        dst_ref=halo,
        send_sem=halo_send,
        recv_sem=halo_recv,
        device_id={"sp": lax.rem(sp + 1, S)},
        device_id_type=MESH,
    )

    @pl.when(sp + 1 < S)
    def _():
        halo_copy.start()

    y_q(0).wait_recv()
    y_q(1).wait_recv()

    log2e = math.log2(math.e)
    coefficient = log2e * HEAD ** (-0.5)
    QT = 256 if R2 % 256 == 0 else 128

    def attend(b, diagonal):
        bias = gate[pl.ds(par, 1), pl.ds(pl.multiple_of(b * R2, 128), R2)] * log2e
        for start in range(0, R2, QT):
            stop = start + QT if diagonal else R2
            rows = pl.ds(start, QT)
            s = lax.dot_general(
                qbuf[rows, :],
                kv[b, 0, pl.ds(0, stop), :],
                (((1,), (1,)), ((), ())),
                preferred_element_type=F32,
            )
            s = s * coefficient - bias[:, :stop]
            if diagonal:
                row = lax.broadcasted_iota(jnp.int32, s.shape, 0) + start
                col = lax.broadcasted_iota(jnp.int32, s.shape, 1)
                s = jnp.where(col <= row, s, -jnp.inf)
                top = jnp.max(s, axis=-1, keepdims=True)
            else:
                before = peak[rows, :]
                top = jnp.maximum(before, jnp.max(s, axis=-1, keepdims=True))
            weight = jnp.exp2(s - top)
            norm = jnp.sum(weight, axis=-1, keepdims=True)
            value = jnp.dot(
                weight.astype(BF16), kv[b, 1, pl.ds(0, stop), :], preferred_element_type=F32
            )
            if not diagonal:
                fade = jnp.exp2(before - top)
                norm = norm + total[rows, :] * fade
                value = value + acc[rows, :] * fade
            peak[rows, :] = top
            total[rows, :] = norm
            acc[rows, :] = value

    attend(g, True)

    arrived_near(3)

    @pl.when(g > 0)
    def _():
        attend(g - 1, False)

    def chain(d, carry):
        for p in range(4):
            arrived(d, p, d < near)
        attend(g - d, False)
        return carry

    lax.fori_loop(2, g + 1, chain, 0)

    gains = head_gain[...].astype(F32).reshape(1, 2 * HEAD)
    gain = jnp.where(par == 0, gains[:, :HEAD], gains[:, HEAD:])

    def finished(block, half):
        rows = pl.ds(pl.multiple_of(block * R + half_start(half), 16), HR)
        return rms(acc[rows, :] / total[rows, :], gain)

    def back(half):
        rows = pl.ds(half_start(half), HR)
        return pltpu.make_async_remote_copy(
            src_ref=ret.at[rows, :],
            dst_ref=heads.at[par, rows, :],
            send_sem=ret_send.at[half],
            recv_sem=ret_recv.at[half],
            device_id={"sp": mate},
            device_id_type=MESH,
        )

    for half in (1, 0):
        ret[pl.ds(pl.multiple_of(half_start(half), 16), HR), :] = finished(1 - par, half)
        back(half).start()
    for half in (1, 0):
        heads[par, pl.ds(pl.multiple_of(half_start(half), 16), HR), :] = finished(par, half)

    @pl.when(sp > 0)
    def _():
        halo_copy.wait_recv()
        padded[0:8, :] = halo[HALO - 8 : HALO, :].astype(F32)

    @pl.when(sp == 0)
    def _():
        padded[0:8, :] = jnp.zeros((8, padded.shape[1]), F32)

    padded[pl.ds(8, R), :] = mixed[...].astype(F32)
    summed = jnp.zeros(mixed.shape, F32)
    for j in range(KTAP):
        summed = summed + taps[j : j + 1, :].astype(F32) * padded[pl.ds(9 - KTAP + j, R), :]
    conv_out = gates[2].astype(F32) * summed
    conv_gain = channel_gain[...].astype(F32).reshape(1, conv_out.shape[1])
    for h in range(conv_out.shape[1] // HEAD):
        cols = slice(h * HEAD, (h + 1) * HEAD)
        group[:, cols] = rms(conv_out[:, cols], conv_gain[:, cols])

    for copy in wo_copies:
        copy.wait()
    back(1).wait_recv()

    NH = out.shape[1] // 2

    def partial(chunk, n):
        rows = pl.ds(pl.multiple_of(chunk * C, 16), C)
        both = jnp.concatenate([heads[0, rows, :], heads[1, rows, :]], axis=1)
        cols = pl.ds(n * NH, NH)
        return jnp.dot(both, wo[0, :, cols], preferred_element_type=F32) + jnp.dot(
            group[rows, :], wo[1, :, cols], preferred_element_type=F32
        )

    def pair_copy(i, n):
        return pltpu.make_async_remote_copy(
            src_ref=part.at[i, n],
            dst_ref=part_in.at[i, n],
            send_sem=pair_send.at[i, n],
            recv_sem=pair_recv.at[i, n],
            device_id={"tp": tp1},
            device_id_type=MESH,
        )

    def x_copy(n):
        return pltpu.make_async_remote_copy(
            src_ref=xsum.at[n],
            dst_ref=xsum_in.at[n],
            send_sem=x_send.at[n],
            recv_sem=x_recv.at[n],
            device_id={"tp": tp2},
            device_id_type=MESH,
        )

    for n in range(2):
        part[0, n] = partial(tp3, n).astype(BF16)
        pair_copy(0, n).start()
    for n in range(2):
        value = partial(tp2, n)
        pair_copy(0, n).wait_recv()
        xsum[n] = (value + part_in[0, n].astype(F32)).astype(BF16)
        x_copy(n).start()
    back(0).wait_recv()
    for n in range(2):
        part[1, n] = partial(tp1, n).astype(BF16)
        pair_copy(1, n).start()
    for n in range(2):
        value = partial(tp, n)
        pair_copy(1, n).wait_recv()
        value = value + part_in[1, n].astype(F32)
        x_copy(n).wait_recv()
        out[:, pl.ds(n * NH, NH)] = (value + xsum_in[n].astype(F32)).astype(BF16)

    cross.wait_send()
    beside.wait_send()
    onward.wait_send()
    for half in range(2):
        y_kv(half).wait_send()
        y_q(half).wait_send()
    back(0).wait_send()
    back(1).wait_send()

    @pl.when(sp + 1 < S)
    def _():
        halo_copy.wait_send()

    for n in range(2):
        x_copy(n).wait_send()
        for i in range(2):
            pair_copy(i, n).wait_send()
    for p in range(4):

        @pl.when(g + 1 < G)
        def _():
            piece_copy(0, p, 1, kv_send.at[0, p]).wait_send()

        for d in range(1, near):

            @pl.when((g + 1 < G) & (g >= d))
            def _():
                piece_copy(d, p, 1, kv_send.at[d, p]).wait_send()

        for step in range(near + 1, G):

            @pl.when(g + step < G)
            def _():
                piece_copy(0, p, step, kv_far.at[step, p]).wait_send()


def local(S, T, tokens, *rest):
    (wq, wk, wv, wgo, wgi, wci, taps, gate, head_gain, channel_gain, wattn, wchan) = rest
    C, D = tokens.shape
    R = C * T
    A = wq.shape[1]
    G = S // 2
    N = wattn.shape[1]
    hbm = pl.BlockSpec(memory_space=pl.ANY)
    vmem = pl.BlockSpec(memory_space=pltpu.VMEM)
    dma = pltpu.SemaphoreType.DMA
    return pl.pallas_call(
        functools.partial(kernel, S, T),
        out_shape=jax.ShapeDtypeStruct((C, N), BF16),
        in_specs=[hbm] * 7 + [vmem] * 4 + [hbm] * 2,
        out_specs=vmem,
        scratch_shapes=[
            pltpu.VMEM((R, D), BF16),
            pltpu.VMEM((6, D, A), BF16),
            pltpu.VMEM((2, A, N), BF16),
            pltpu.VMEM((G, 2, 2 * R, HEAD), BF16),
            pltpu.VMEM((2 * R, HEAD), BF16),
            pltpu.VMEM((2, R, HEAD), BF16),
            pltpu.VMEM((R, HEAD), BF16),
            pltpu.VMEM((3, R, A), BF16),
            pltpu.VMEM((R, A), BF16),
            pltpu.VMEM((HALO, A), BF16),
            pltpu.VMEM((R + 8, A), F32),
            pltpu.VMEM((R, A), BF16),
            pltpu.VMEM((2 * R, 1), F32),
            pltpu.VMEM((2 * R, 1), F32),
            pltpu.VMEM((2 * R, HEAD), F32),
            pltpu.VMEM((R, HEAD), BF16),
            pltpu.VMEM((2, R, HEAD), BF16),
            pltpu.VMEM((2, 2, C, N // 2), BF16),
            pltpu.VMEM((2, 2, C, N // 2), BF16),
            pltpu.VMEM((2, C, N // 2), BF16),
            pltpu.VMEM((2, C, N // 2), BF16),
            dma((6,)),
            dma((2,)),
            dma,
            dma((3,)),
            dma((3,)),
            dma((2, 2)),
            dma((2, 2)),
            dma((G, 4)),
            dma((G, 4)),
            dma((G + 1, 4)),
            dma,
            dma,
            dma((2,)),
            dma((2,)),
            dma((2, 2)),
            dma((2, 2)),
            dma((2,)),
            dma((2,)),
        ],
        compiler_params=pltpu.CompilerParams(
            collective_id=0, has_side_effects=True, vmem_limit_bytes=60 * 1024 * 1024
        ),
    )(
        tokens,
        wq,
        wk,
        wv,
        wgo,
        wgi,
        wci,
        taps,
        gate,
        head_gain,
        channel_gain,
        wattn,
        wchan,
    )


def solution(mesh):
    S, T = mesh.shape["sp"], mesh.shape["tp"]
    cols = P(None, "tp")
    rows = P("tp", None)
    placed = (
        (P(("sp", "tp"), None),) + (cols,) * 7 + (rows, P("tp"), P("tp")) + (rows, rows)
    )
    return jax.shard_map(
        functools.partial(local, S, T),
        mesh=mesh,
        in_specs=placed,
        out_specs=P(("sp", "tp"), None),
        check_vma=False,
    )
```

```python
import functools
import math

import jax
import jax.numpy as jnp
from jax import lax
from jax.experimental import pallas as pl
from jax.experimental.pallas import tpu as pltpu
from jax.sharding import PartitionSpec as P

HEAD = 128
KTAP = 3
HALO = 16
MESH = pl.DeviceIdType.MESH
F32 = jnp.float32
BF16 = jnp.bfloat16


def rms(values, gain):
    scale = lax.rsqrt(jnp.mean(values * values, axis=-1, keepdims=True) + 1e-06)
    return (values * scale * gain).astype(BF16)


def kernel(
    S,
    T,
    tokens,
    wq,
    wk,
    wv,
    wgo,
    wgi,
    wci,
    taps,
    gate,
    head_gain,
    channel_gain,
    wattn,
    wchan,
    out,
    tok,
    w,
    wo,
    kv,
    qbuf,
    stage_kv,
    stage_q,
    gates,
    mixed,
    halo,
    padded,
    group,
    peak,
    total,
    acc,
    ret,
    heads,
    part,
    part_in,
    xsum,
    xsum_in,
    chan,
    kept,
    w_sem,
    wo_sem,
    tok_sem,
    tok_send,
    tok_recv,
    y_send,
    y_recv,
    kv_send,
    kv_recv,
    halo_send,
    halo_recv,
    ret_send,
    ret_recv,
    pair_send,
    pair_recv,
    x_send,
    x_recv,
):
    sp = lax.axis_index("sp")
    tp = lax.axis_index("tp")
    G = S // 2
    g = sp // 2
    par = sp % 2
    mate = sp + 1 - 2 * par
    C = tokens.shape[0]
    R = C * T
    HR = R // 2
    R2 = 2 * R
    pair = tp // 2
    tp1 = tp + 1 - 2 * (tp % 2)
    tp2 = (tp + 2) % T
    tp3 = (tp1 + 2) % T
    near = G - 1
    forwards = g + 1 < G

    weights = (wk, wv, wq, wgi, wci, wgo)
    own_copy = pltpu.make_async_copy(tokens, tok.at[pl.ds(tp * C, C)], tok_sem)
    own_copy.start()
    w_copies = [pltpu.make_async_copy(weights[i], w.at[i], w_sem.at[i]) for i in range(6)]
    for copy in w_copies[:3]:
        copy.start()
    wo_copies = [
        pltpu.make_async_copy(ref, wo.at[i], wo_sem.at[i]) for i, ref in enumerate((wattn, wchan))
    ]

    barrier = pltpu.get_barrier_semaphore()
    for o in range(1, T):
        pl.semaphore_signal(barrier, inc=1, device_id={"tp": (tp + o) % T}, device_id_type=MESH)
    for o in range(1, S):
        pl.semaphore_signal(barrier, inc=1, device_id={"sp": (sp + o) % S}, device_id_type=MESH)
    pl.semaphore_wait(barrier, S + T - 2)

    def tok_copy(slot, target, index):
        rows = pl.ds(slot * C, C)
        return pltpu.make_async_remote_copy(
            src_ref=tok.at[rows],
            dst_ref=tok.at[rows],
            send_sem=tok_send.at[index],
            recv_sem=tok_recv.at[index],
            device_id={"tp": target},
            device_id_type=MESH,
        )

    own_copy.wait()
    cross = tok_copy(tp, tp2, 0)
    cross.start()
    beside = tok_copy(tp, tp1, 1)
    beside.start()
    for copy in w_copies[3:] + wo_copies:
        copy.start()

    def half_start(half):
        return (pair if half == 0 else 1 - pair) * HR

    def y_kv(half):
        rs = half_start(half)
        return pltpu.make_async_remote_copy(
            src_ref=stage_kv.at[:, pl.ds(rs, HR), :],
            dst_ref=kv.at[g, :, pl.ds(par * R + rs, HR), :],
            send_sem=y_send.at[half, 0],
            recv_sem=y_recv.at[half, 0],
            device_id={"sp": mate},
            device_id_type=MESH,
        )

    def y_q(half):
        rs = half_start(half)
        return pltpu.make_async_remote_copy(
            src_ref=stage_q.at[pl.ds(rs, HR), :],
            dst_ref=qbuf.at[pl.ds(par * R + rs, HR), :],
            send_sem=y_send.at[half, 1],
            recv_sem=y_recv.at[half, 1],
            device_id={"sp": mate},
            device_id_type=MESH,
        )

    def piece_copy(d, p, step, send_sem):
        half, other = p // 2, p % 2
        rows = pl.ds((1 - par if other else par) * R + half_start(half), HR)
        ref = kv.at[g - d, :, rows, :]
        return pltpu.make_async_remote_copy(
            src_ref=ref,
            dst_ref=ref,
            send_sem=send_sem,
            recv_sem=kv_recv.at[d + step, p],
            device_id={"sp": lax.rem(sp + 2 * step, S)},
            device_id_type=MESH,
        )

    def send_own(p):
        @pl.when(g + 1 < G)
        def _():
            piece_copy(0, p, 1, kv_send.at[0, p]).start()

    def arrived(d, p, send_on):
        piece_copy(d, p, 0, kv_send.at[d, p]).wait_recv()

        @pl.when(jnp.logical_and(send_on, g + 1 < G))
        def _():
            piece_copy(d, p, 1, kv_send.at[d, p]).start()

    def early(d, p):
        if d < near:

            @pl.when((g >= d) & forwards)
            def _():
                arrived(d, p, True)

    def late(d, p):
        if d < near:

            @pl.when(jnp.logical_not(forwards))
            def _():
                arrived(d, p, False)

        else:
            arrived(d, p, False)

    def project(half, index):
        rs = pl.multiple_of(half_start(half), 16)
        rows = tok[pl.ds(rs, HR), :]
        return rs, jnp.dot(rows, w[index], preferred_element_type=F32).astype(BF16)

    def split(value):
        a, b = value[:, :HEAD], value[:, HEAD:]
        return jnp.where(par == 0, a, b), jnp.where(par == 0, b, a)

    def attention_inputs(half):
        for i in range(2):
            if half == 0:
                w_copies[i].wait()
            rs, value = project(half, i)
            mine, theirs = split(value)
            kv[g, i, pl.ds(pl.multiple_of(par * R + rs, 16), HR), :] = mine
            stage_kv[i, pl.ds(rs, HR), :] = theirs
        y_kv(half).start()
        send_own(2 * half)
        if half == 0:
            w_copies[2].wait()
        rs, value = project(half, 2)
        mine, theirs = split(value)
        qbuf[pl.ds(pl.multiple_of(par * R + rs, 16), HR), :] = mine
        stage_q[pl.ds(rs, HR), :] = theirs
        y_q(half).start()

    def gate_inputs(half):
        for i in range(3, 6):
            if half == 0:
                w_copies[i].wait()
            rs, value = project(half, i)
            gates[i - 3, pl.ds(rs, HR), :] = value

    beside.wait_recv()
    attention_inputs(0)
    gate_inputs(0)
    y_kv(0).wait_recv()
    send_own(1)
    early(1, 0)

    tok_copy(tp2, tp2, 0).wait_recv()
    onward = tok_copy(tp2, tp1, 2)
    onward.start()
    tok_copy(tp3, tp1, 2).wait_recv()
    attention_inputs(1)
    early(1, 1)
    gate_inputs(1)
    early(2, 0)
    y_kv(1).wait_recv()
    send_own(3)
    early(1, 2)
    early(2, 1)

    mixed[...] = (gates[0].astype(F32) * gates[1].astype(F32)).astype(BF16)
    halo_copy = pltpu.make_async_remote_copy(
        src_ref=mixed.at[pl.ds(R - HALO, HALO), :],
        dst_ref=halo,
        send_sem=halo_send,
        recv_sem=halo_recv,
        device_id={"sp": lax.rem(sp + 1, S)},
        device_id_type=MESH,
    )

    @pl.when(sp + 1 < S)
    def _():
        halo_copy.start()

    y_q(0).wait_recv()
    y_q(1).wait_recv()

    log2e = math.log2(math.e)
    coefficient = log2e * HEAD ** (-0.5)
    QT = 256 if R2 % 256 == 0 else 128

    def attend(b, diagonal):
        bias = gate[pl.ds(par, 1), pl.ds(pl.multiple_of(b * R2, 128), R2)] * log2e
        for start in range(0, R2, QT):
            stop = start + QT if diagonal else R2
            rows = pl.ds(start, QT)
            s = lax.dot_general(
                qbuf[rows, :],
                kv[b, 0, pl.ds(0, stop), :],
                (((1,), (1,)), ((), ())),
                preferred_element_type=F32,
            )
            s = s * coefficient - bias[:, :stop]
            if diagonal:
                row = lax.broadcasted_iota(jnp.int32, s.shape, 0) + start
                col = lax.broadcasted_iota(jnp.int32, s.shape, 1)
                s = jnp.where(col <= row, s, -jnp.inf)
                top = jnp.max(s, axis=-1, keepdims=True)
            else:
                before = peak[rows, :]
                top = jnp.maximum(before, jnp.max(s, axis=-1, keepdims=True))
            weight = jnp.exp2(s - top)
            norm = jnp.sum(weight, axis=-1, keepdims=True)
            value = jnp.dot(
                weight.astype(BF16), kv[b, 1, pl.ds(0, stop), :], preferred_element_type=F32
            )
            if not diagonal:
                fade = jnp.exp2(before - top)
                norm = norm + total[rows, :] * fade
                value = value + acc[rows, :] * fade
            peak[rows, :] = top
            total[rows, :] = norm
            acc[rows, :] = value

    attend(g, True)

    early(1, 3)
    early(2, 2)

    @pl.when(g >= 1)
    def _():
        for p in range(4):
            late(1, p)
        attend(g - 1, False)

    early(2, 3)

    @pl.when(g >= 2)
    def _():
        for p in range(4):
            late(2, p)
        attend(g - 2, False)

    def chain(d, carry):
        for p in range(4):
            arrived(d, p, d < near)
        attend(g - d, False)
        return carry

    lax.fori_loop(3, g + 1, chain, 0)

    gains = head_gain[...].astype(F32).reshape(1, 2 * HEAD)
    gain = jnp.where(par == 0, gains[:, :HEAD], gains[:, HEAD:])

    def finished(block, half):
        rows = pl.ds(pl.multiple_of(block * R + half_start(half), 16), HR)
        return rms(acc[rows, :] / total[rows, :], gain)

    def back(half):
        rows = pl.ds(half_start(half), HR)
        return pltpu.make_async_remote_copy(
            src_ref=ret.at[rows, :],
            dst_ref=heads.at[par, rows, :],
            send_sem=ret_send.at[half],
            recv_sem=ret_recv.at[half],
            device_id={"sp": mate},
            device_id_type=MESH,
        )

    for half in (1, 0):
        ret[pl.ds(pl.multiple_of(half_start(half), 16), HR), :] = finished(1 - par, half)
        back(half).start()
    for half in (1, 0):
        heads[par, pl.ds(pl.multiple_of(half_start(half), 16), HR), :] = finished(par, half)

    @pl.when(sp > 0)
    def _():
        halo_copy.wait_recv()
        padded[0:8, :] = halo[HALO - 8 : HALO, :].astype(F32)

    @pl.when(sp == 0)
    def _():
        padded[0:8, :] = jnp.zeros((8, padded.shape[1]), F32)

    padded[pl.ds(8, R), :] = mixed[...].astype(F32)
    summed = jnp.zeros(mixed.shape, F32)
    for j in range(KTAP):
        summed = summed + taps[j : j + 1, :].astype(F32) * padded[pl.ds(9 - KTAP + j, R), :]
    conv_out = gates[2].astype(F32) * summed
    conv_gain = channel_gain[...].astype(F32).reshape(1, conv_out.shape[1])
    for h in range(conv_out.shape[1] // HEAD):
        cols = slice(h * HEAD, (h + 1) * HEAD)
        group[:, cols] = rms(conv_out[:, cols], conv_gain[:, cols])

    for copy in wo_copies:
        copy.wait()
    NS = part.shape[1]
    NH = out.shape[1] // NS
    for n in range(NS):
        cols = pl.ds(n * NH, NH)
        chan[:, cols] = jnp.dot(group[...], wo[1, :, cols], preferred_element_type=F32)
    back(1).wait_recv()

    def partial(half, n):
        rows = pl.ds(pl.multiple_of(half_start(half), 16), HR)
        both = jnp.concatenate([heads[0, rows, :], heads[1, rows, :]], axis=1)
        cols = pl.ds(n * NH, NH)
        value = jnp.dot(both, wo[0, :, cols], preferred_element_type=F32) + chan[rows, cols]
        a, b = value[:C], value[C:]
        first = tp % 2 == 0
        return jnp.where(first, a, b), jnp.where(first, b, a)

    def pair_copy(i, n):
        return pltpu.make_async_remote_copy(
            src_ref=part.at[i, n],
            dst_ref=part_in.at[i, n],
            send_sem=pair_send.at[i, n],
            recv_sem=pair_recv.at[i, n],
            device_id={"tp": tp1},
            device_id_type=MESH,
        )

    def x_copy(n):
        return pltpu.make_async_remote_copy(
            src_ref=xsum.at[n],
            dst_ref=xsum_in.at[n],
            send_sem=x_send.at[n],
            recv_sem=x_recv.at[n],
            device_id={"tp": tp2},
            device_id_type=MESH,
        )

    for n in range(NS):
        mine, theirs = partial(1, n)
        part[0, n] = theirs.astype(BF16)
        pair_copy(0, n).start()
        kept[n] = mine
    for n in range(NS):
        pair_copy(0, n).wait_recv()
        xsum[n] = (kept[n] + part_in[0, n].astype(F32)).astype(BF16)
        x_copy(n).start()
    back(0).wait_recv()
    for n in range(NS):
        mine, theirs = partial(0, n)
        part[1, n] = theirs.astype(BF16)
        pair_copy(1, n).start()
        kept[n] = mine
    for n in range(NS):
        pair_copy(1, n).wait_recv()
        kept[n] = kept[n] + part_in[1, n].astype(F32)
    for n in range(NS):
        x_copy(n).wait_recv()
        out[:, pl.ds(n * NH, NH)] = (kept[n] + xsum_in[n].astype(F32)).astype(BF16)

    cross.wait_send()
    beside.wait_send()
    onward.wait_send()
    for half in range(2):
        y_kv(half).wait_send()
        y_q(half).wait_send()
    back(0).wait_send()
    back(1).wait_send()

    @pl.when(sp + 1 < S)
    def _():
        halo_copy.wait_send()

    for n in range(NS):
        x_copy(n).wait_send()
        for i in range(2):
            pair_copy(i, n).wait_send()
    for p in range(4):

        @pl.when(g + 1 < G)
        def _():
            piece_copy(0, p, 1, kv_send.at[0, p]).wait_send()

        for d in range(1, near):

            @pl.when((g + 1 < G) & (g >= d))
            def _():
                piece_copy(d, p, 1, kv_send.at[d, p]).wait_send()


def local(S, T, tokens, *rest):
    (wq, wk, wv, wgo, wgi, wci, taps, gate, head_gain, channel_gain, wattn, wchan) = rest
    C, D = tokens.shape
    R = C * T
    A = wq.shape[1]
    G = S // 2
    N = wattn.shape[1]
    NS = 4
    hbm = pl.BlockSpec(memory_space=pl.ANY)
    vmem = pl.BlockSpec(memory_space=pltpu.VMEM)
    dma = pltpu.SemaphoreType.DMA
    return pl.pallas_call(
        functools.partial(kernel, S, T),
        out_shape=pltpu.VMEM((C, N), BF16),
        in_specs=[hbm] * 7 + [vmem] * 4 + [hbm] * 2,
        out_specs=vmem,
        scratch_shapes=[
            pltpu.VMEM((R, D), BF16),
            pltpu.VMEM((6, D, A), BF16),
            pltpu.VMEM((2, A, N), BF16),
            pltpu.VMEM((G, 2, 2 * R, HEAD), BF16),
            pltpu.VMEM((2 * R, HEAD), BF16),
            pltpu.VMEM((2, R, HEAD), BF16),
            pltpu.VMEM((R, HEAD), BF16),
            pltpu.VMEM((3, R, A), BF16),
            pltpu.VMEM((R, A), BF16),
            pltpu.VMEM((HALO, A), BF16),
            pltpu.VMEM((R + 8, A), F32),
            pltpu.VMEM((R, A), BF16),
            pltpu.VMEM((2 * R, 1), F32),
            pltpu.VMEM((2 * R, 1), F32),
            pltpu.VMEM((2 * R, HEAD), F32),
            pltpu.VMEM((R, HEAD), BF16),
            pltpu.VMEM((2, R, HEAD), BF16),
            pltpu.VMEM((2, NS, C, N // NS), BF16),
            pltpu.VMEM((2, NS, C, N // NS), BF16),
            pltpu.VMEM((NS, C, N // NS), BF16),
            pltpu.VMEM((NS, C, N // NS), BF16),
            pltpu.VMEM((R, N), F32),
            pltpu.VMEM((NS, C, N // NS), F32),
            dma((6,)),
            dma((2,)),
            dma,
            dma((3,)),
            dma((3,)),
            dma((2, 2)),
            dma((2, 2)),
            dma((G, 4)),
            dma((G, 4)),
            dma,
            dma,
            dma((2,)),
            dma((2,)),
            dma((2, NS)),
            dma((2, NS)),
            dma((NS,)),
            dma((NS,)),
        ],
        compiler_params=pltpu.CompilerParams(
            collective_id=0, has_side_effects=True, vmem_limit_bytes=60 * 1024 * 1024
        ),
    )(
        tokens,
        wq,
        wk,
        wv,
        wgo,
        wgi,
        wci,
        taps,
        gate,
        head_gain,
        channel_gain,
        wattn,
        wchan,
    )


def solution(mesh):
    S, T = mesh.shape["sp"], mesh.shape["tp"]
    cols = P(None, "tp")
    rows = P("tp", None)
    placed = (
        (P(("sp", "tp"), None),) + (cols,) * 7 + (rows, P("tp"), P("tp")) + (rows, rows)
    )
    return jax.shard_map(
        functools.partial(local, S, T),
        mesh=mesh,
        in_specs=placed,
        out_specs=P(("sp", "tp"), None),
        check_vma=False,
    )
```
